32 devices in a mesh: tp: 4 (over z), dp: 8 (over y, x, core).
Axes of the slice: x: 2, y: 2, z: 4, core: 2. Of those that a mesh axis runs over, the one named last changes fastest.
Arguments:
- tokens: bfloat16 [64, 4096], P(None, 'dp'), may hold values from -6 to 6
- norm_gain: float32 [2, 4096], P(None, 'dp'), may hold values from 0.1 to 1.9
- w_gate: bfloat16 [2, 4096, 3072], P(None, 'dp', 'tp'), may hold values from -0.09375 to 0.09375
- w_value: bfloat16 [2, 4096, 3072], P(None, 'dp', 'tp'), may hold values from -0.09375 to 0.09375
- w_inmap: bfloat16 [2, 4096, 3072], P(None, 'dp', 'tp'), may hold values from -0.09375 to 0.09375
- w_readout: bfloat16 [2, 4096, 3072], P(None, 'dp', 'tp'), may hold values from -0.09375 to 0.09375
- w_step: bfloat16 [2, 4096, 48], P(None, 'dp'), may hold values from -0.09375 to 0.09375
- step_bias: float32 [2, 48], P(None, 'tp'), may hold values from -4 to 1
- decay_log: float32 [2, 48], P(None, 'tp'), may hold values from -1 to 2.5
- skip_gain: float32 [2, 48], P(None, 'tp'), may hold values from 0.5 to 2
- conv_taps: bfloat16 [2, 5, 3, 3072], P(None, None, None, 'tp'), may hold values from -2.5 to 2.5
- gate_gain: float32 [2, 3072], P(None, 'tp'), may hold values from 0.1 to 1.9
- w_project: bfloat16 [2, 3072, 4096], P(None, 'tp', 'dp'), may hold values from -0.109375 to 0.109375
- states: float32 [2, 64, 48, 4096], P(None, 'dp', 'tp'), may hold values from -3 to 3
- recent: bfloat16 [2, 64, 4, 3, 3072], P(None, 'dp', None, None, 'tp'), may hold values from -6 to 6
Outputs:
- next_tokens: bfloat16 [64, 4096], P(None, 'dp')
- next_states: float32 [2, 64, 48, 4096], P(None, 'dp', 'tp')
- next_recent: bfloat16 [2, 64, 4, 3, 3072], P(None, 'dp', None, None, 'tp')
The draws below stay inside these ranges and needn't reach their ends.
All inputs are finite; a program needn't handle non-finite values.
Results may differ from the reference program's by a relative error of at most 0.014.
Values may be sent and summed in bfloat16 or wider, within the bound.
No kernel may reach another device: no remote copies, remote signals or barrier semaphores. Data moves between devices by JAX's collectives and lax.ppermute only.
A program may use at most 64 MiB of HBM per device.

```python
import jax
import jax.numpy as jnp
from jax import lax

D = 4096
HEADS = 48
HEAD_DIM = 64
STATE = 64
SSD_DIM = 3072
CONV = 5
LAYERS = 2
BATCH = 64


def shard_levels(stream_key, extent, split, low, high):
    loudness = 1.0
    for position, shards_of in split:
        heights = jax.random.uniform(jax.random.fold_in(jax.random.fold_in(stream_key, 6), position), (shards_of,), jnp.float32, low / len(split), high / len(split))
        loudness = loudness * jnp.repeat(jnp.exp(heights), extent[position] // shards_of).reshape((-1,) + (1,) * (len(extent) - 1 - position))
    return loudness


def scatter_about(own_key, extent, deviation, bound, split=(), dtype=jnp.bfloat16):
    values = jax.random.normal(own_key, extent, jnp.float32) * deviation
    if len(split) > 0:
        values = shard_levels(own_key, extent, split, -0.22, 0.18) * values
    return jnp.clip(values, min=-bound, max=bound).astype(dtype)


def setup_inputs(seed: int = 0) -> dict:
    key_of = jax.random.split(jax.random.key(seed), 16)
    return {
        "tokens": scatter_about(key_of[0], (BATCH, D), 1.0, 6.0, ((1, 8),)),
        "norm_gain": jnp.clip(1.0 + 0.18 * jax.random.normal(key_of[1], (LAYERS, D), jnp.float32), 0.1, 1.9),
        "w_gate": scatter_about(key_of[2], (LAYERS, D, SSD_DIM), D ** -0.5, 0.09375, ((1, 8), (2, 4))),
        "w_value": scatter_about(key_of[3], (LAYERS, D, SSD_DIM), D ** -0.5, 0.09375, ((1, 8), (2, 4))),
        "w_inmap": scatter_about(key_of[4], (LAYERS, D, SSD_DIM), D ** -0.5, 0.09375, ((1, 8), (2, 4))),
        "w_readout": scatter_about(key_of[5], (LAYERS, D, SSD_DIM), D ** -0.5, 0.09375, ((1, 8), (2, 4))),
        "w_step": scatter_about(key_of[6], (LAYERS, D, HEADS), D ** -0.5, 0.09375, ((1, 8),)),
        "step_bias": jnp.clip(-4.0 + 5.0 * jax.random.uniform(key_of[7], (LAYERS, HEADS), jnp.float32) ** shard_levels(key_of[7], (LAYERS, HEADS), ((1, 4),), -0.2, 0.2), -4.0, 1.0),
        "decay_log": jnp.clip(-1.0 + 3.5 * jax.random.uniform(key_of[8], (LAYERS, HEADS), jnp.float32) ** shard_levels(key_of[8], (LAYERS, HEADS), ((1, 4),), -0.2, 0.2), -1.0, 2.5),
        "skip_gain": jnp.clip(0.5 + 1.5 * jax.random.uniform(key_of[9], (LAYERS, HEADS), jnp.float32) ** shard_levels(key_of[9], (LAYERS, HEADS), ((1, 4),), -0.2, 0.2), 0.5, 2.0),
        "conv_taps": scatter_about(key_of[10], (LAYERS, CONV, 3, SSD_DIM), CONV ** -0.5, 2.5, ((3, 4),)),
        "gate_gain": jnp.clip(1.0 + 0.18 * jax.random.normal(key_of[11], (LAYERS, SSD_DIM), jnp.float32), 0.1, 1.9),
        "w_project": scatter_about(key_of[12], (LAYERS, SSD_DIM, D), SSD_DIM ** -0.5, 0.109375, ((1, 4), (2, 8))),
        "states": scatter_about(key_of[13], (LAYERS, BATCH, HEADS, HEAD_DIM * STATE), 0.5, 3.0, ((1, 8), (2, 4)), jnp.float32),
        "recent": scatter_about(key_of[14], (LAYERS, BATCH, CONV - 1, 3, SSD_DIM), 1.0, 6.0, ((1, 8), (4, 4))),
    }


EPS = 1e-06

def run_block(tokens_now, level, norm_gain, w_gate, w_value, w_inmap, w_readout, w_step, step_bias, decay_log, skip_gain, conv_taps, gate_gain, w_project, states, recent):
    tokens_f = tokens_now.astype(jnp.float32)
    scale_one = lax.rsqrt(lax.optimization_barrier(jnp.mean(tokens_f * tokens_f, axis=-1, keepdims=True)) + EPS)
    gained = (tokens_f * norm_gain[level][None, :]).astype(jnp.bfloat16)

    def project(weight):
        return scale_one * jnp.dot(gained, weight[level], preferred_element_type=jnp.float32)
    gate_pre = project(w_gate)
    step_raw = project(w_step)
    stacked = jnp.stack([project(w_value), project(w_inmap), project(w_readout)], axis=1).astype(jnp.bfloat16)
    window = jnp.concatenate([recent[level], stacked[:, None]], axis=1)
    taps_sum = lax.optimization_barrier(jnp.sum(window.astype(jnp.float32) * conv_taps[level].astype(jnp.float32)[None], axis=1))
    active = jax.nn.silu(taps_sum)
    rows = tokens_now.shape[0]
    x_value = active[:, 0].reshape(rows, HEADS, HEAD_DIM)
    in_map = active[:, 1].reshape(rows, HEADS, STATE)
    out_map = active[:, 2].reshape(rows, HEADS, STATE)
    step_size = jax.nn.softplus(step_raw + step_bias[level][None, :])
    decay_rate = jnp.exp(-step_size * jnp.exp(decay_log[level])[None, :])
    old_state = states[level].reshape(rows, HEADS, HEAD_DIM, STATE)
    fresh = decay_rate[:, :, None, None] * old_state + (step_size[:, :, None] * x_value)[:, :, :, None] * in_map[:, :, None, :]
    head_out = jnp.einsum('bhpn,bhn->bhp', fresh, out_map) + skip_gain[level][None, :, None] * x_value
    gated = (head_out.reshape(rows, SSD_DIM) * jax.nn.silu(gate_pre) * gate_gain[level][None, :]).astype(jnp.bfloat16)
    gated_f = gated.astype(jnp.float32)
    scale_two = lax.rsqrt(lax.optimization_barrier(jnp.mean(gated_f * gated_f, axis=-1, keepdims=True)) + EPS)
    mixed_out = scale_two * jnp.dot(gated, w_project[level], preferred_element_type=jnp.float32)
    return ((tokens_f + mixed_out).astype(jnp.bfloat16), fresh.reshape(rows, HEADS, HEAD_DIM * STATE), window[:, 1:])

def reference(tokens, norm_gain, w_gate, w_value, w_inmap, w_readout, w_step, step_bias, decay_log, skip_gain, conv_taps, gate_gain, w_project, states, recent):
    current = tokens
    state_list = []
    recent_list = []
    for level in range(LAYERS):
        current, fresh, kept = run_block(current, level, norm_gain, w_gate, w_value, w_inmap, w_readout, w_step, step_bias, decay_log, skip_gain, conv_taps, gate_gain, w_project, states, recent)
        state_list.append(fresh)
        recent_list.append(kept)
    return (current, jnp.stack(state_list, axis=0), jnp.stack(recent_list, axis=0))
```

```python
import jax
import jax.numpy as jnp
from jax import lax
from jax.sharding import PartitionSpec as P

EPS = 1e-06
AUX = 128


def swap(value, axis, mask):
    count = lax.axis_size(axis)
    return lax.ppermute(value, axis, [(i, i ^ mask) for i in range(count)])


def split_two(value):
    high = value.astype(jnp.bfloat16)
    low = (value - high.astype(jnp.float32)).astype(jnp.bfloat16)
    return high, low


def scatter_sum(total, own):
    group = lax.axis_size("dp")
    half = group // 2
    from_mate = swap(total[half * own :], "dp", 1)
    chip_sum = total[: half * own].astype(jnp.float32) + from_mate.astype(jnp.float32)
    chip_sum = chip_sum.astype(jnp.bfloat16).reshape(half, own, -1)
    parts = [swap(chip_sum[k], "dp", 2 * k + 1) for k in reversed(range(half))]
    return sum(part.astype(jnp.float32) for part in parts)


def sum_tp(value):
    count = lax.axis_size("tp")
    if count & (count - 1) or count > 8:
        return lax.psum(value.astype(jnp.float32), "tp")
    terms = [value] + [None] * (count - 1)
    for mask in sorted(range(1, count), reverse=True):
        terms[mask] = swap(value, "tp", mask)
    terms = [term.astype(jnp.float32) for term in terms]
    while len(terms) > 1:
        terms = [a + b for a, b in zip(terms[::2], terms[1::2])]
    return terms[0]


def per_device(
    tokens,
    norm_gain,
    w_gate,
    w_value,
    w_inmap,
    w_readout,
    w_step,
    step_bias,
    decay_log,
    skip_gain,
    conv_taps,
    gate_gain,
    w_project,
    states,
    recent,
):
    group = lax.axis_size("dp")
    width = tokens.shape[1] * group
    layers, own, heads, cells = states.shape
    channels = w_gate.shape[2]
    inner = channels * lax.axis_size("tp")
    head_dim = channels // heads
    state = cells // head_dim
    me = lax.axis_index("dp")
    first_head = lax.axis_index("tp") * heads
    half = group // 2
    order = [2 * k + 1 for k in range(half)] + [2 * k for k in range(half)]
    w_step_own = lax.dynamic_slice_in_dim(w_step, first_head, heads, 2)

    current = tokens
    state_list = []
    recent_list = []
    for level in range(layers):
        tokens_f = current.astype(jnp.float32)
        blocks = tokens_f.reshape(group, own, -1)
        rows = jnp.concatenate(
            [lax.dynamic_index_in_dim(blocks, me ^ mask, 0, keepdims=False) for mask in order]
        )
        gained = (rows * norm_gain[level][None, :]).astype(jnp.bfloat16)

        def project(weight):
            return jnp.dot(gained, weight, preferred_element_type=jnp.float32)

        square = jnp.sum(rows * rows, axis=1, keepdims=True)
        aux = jnp.concatenate([project(w_step_own[level]), square], axis=1)
        high, low = split_two(aux)
        pad = jnp.zeros((rows.shape[0], AUX - 2 * heads - 2), jnp.bfloat16)
        total = jnp.concatenate(
            [
                project(weight[level]).astype(jnp.bfloat16)
                for weight in (w_gate, w_value, w_inmap, w_readout)
            ]
            + [high, low, pad],
            axis=1,
        )
        mine = scatter_sum(total, own)
        tail = mine[:, 4 * channels :]
        aux = tail[:, : heads + 1] + tail[:, heads + 1 : 2 * heads + 2]
        scale_one = lax.rsqrt(aux[:, heads:] / width + EPS)
        scaled = scale_one * mine[:, : 4 * channels]
        gate_pre = scaled[:, :channels]
        stacked = scaled[:, channels:].reshape(own, 3, channels).astype(jnp.bfloat16)
        window = jnp.concatenate([recent[level], stacked[:, None]], axis=1)
        taps_sum = jnp.sum(
            window.astype(jnp.float32) * conv_taps[level].astype(jnp.float32)[None], axis=1
        )
        active = jax.nn.silu(taps_sum)
        x_value = active[:, 0].reshape(own, heads, head_dim)
        in_map = active[:, 1].reshape(own, heads, state)
        out_map = active[:, 2].reshape(own, heads, state)
        step_raw = scale_one * aux[:, :heads]
        step_size = jax.nn.softplus(step_raw + step_bias[level][None, :])
        decay_rate = jnp.exp(-step_size * jnp.exp(decay_log[level])[None, :])
        old_state = states[level].reshape(own, heads, head_dim, state)
        fresh = (
            decay_rate[:, :, None, None] * old_state
            + (step_size[:, :, None] * x_value)[:, :, :, None] * in_map[:, :, None, :]
        )
        head_out = (
            jnp.einsum("bhpn,bhn->bhp", fresh, out_map) + skip_gain[level][None, :, None] * x_value
        )
        gated = (
            head_out.reshape(own, channels) * jax.nn.silu(gate_pre) * gate_gain[level][None, :]
        ).astype(jnp.bfloat16)
        copies = jnp.broadcast_to(gated[None], (group, own, channels))
        all_gated = lax.all_to_all(copies, "dp", 0, 0, tiled=True).reshape(group * own, channels)
        gated_f = all_gated.astype(jnp.float32)
        part_two = jnp.sum(gated_f * gated_f, axis=1, keepdims=True)
        partial_out = jnp.dot(all_gated, w_project[level], preferred_element_type=jnp.float32)
        high, low = split_two(part_two)
        pad = jnp.zeros((rows.shape[0], AUX - 2), jnp.bfloat16)
        summed = sum_tp(
            jnp.concatenate([partial_out.astype(jnp.bfloat16), high, low, pad], axis=1)
        )
        out_cols = partial_out.shape[1]
        square_two = summed[:, out_cols : out_cols + 1] + summed[:, out_cols + 1 : out_cols + 2]
        scale_two = lax.rsqrt(square_two / inner + EPS)
        current = (tokens_f + scale_two * summed[:, :out_cols]).astype(jnp.bfloat16)
        state_list.append(fresh.reshape(own, heads, cells))
        recent_list.append(window[:, 1:])
    return (current, jnp.stack(state_list, axis=0), jnp.stack(recent_list, axis=0))


def solution(mesh):
    in_specs = (
        P(None, "dp"),
        P(None, "dp"),
        P(None, "dp", "tp"),
        P(None, "dp", "tp"),
        P(None, "dp", "tp"),
        P(None, "dp", "tp"),
        P(None, "dp", None),
        P(None, "tp"),
        P(None, "tp"),
        P(None, "tp"),
        P(None, None, None, "tp"),
        P(None, "tp"),
        P(None, "tp", "dp"),
        P(None, "dp", "tp", None),
        P(None, "dp", None, None, "tp"),
    )
    out_specs = (P(None, "dp"), P(None, "dp", "tp", None), P(None, "dp", None, None, "tp"))
    return jax.shard_map(
        per_device, mesh=mesh, in_specs=in_specs, out_specs=out_specs, check_vma=False
    )
```

```python
import functools

import jax
import jax.numpy as jnp
from jax import lax
from jax.experimental import pallas as pl
from jax.experimental.pallas import tpu as pltpu
from jax.sharding import PartitionSpec as P

EPS = 1e-06
LANES = 128
HALF = LANES // 2

VMEM = pl.BlockSpec(memory_space=pltpu.VMEM)
F32 = jnp.float32
BF16 = jnp.bfloat16


HBM = pl.BlockSpec(memory_space=pltpu.HBM)


def call(kernel, outs, args, flops, scratch=(), limit=8 << 20, far=(), far_out=(), alias={}):
    moved = sum(a.size * a.dtype.itemsize for a in (*args, *outs))
    args = [
        pltpu.with_memory_space_constraint(a, pltpu.HBM if k in far else pltpu.VMEM)
        for k, a in enumerate(args)
    ]
    places = [pltpu.HBM if k in far_out else pltpu.VMEM for k in range(len(outs))]
    return pl.pallas_call(
        kernel,
        out_shape=[place(out.shape, out.dtype) for place, out in zip(places, outs)],
        in_specs=[HBM if k in far else VMEM for k in range(len(args))],
        out_specs=[HBM if k in far_out else VMEM for k in range(len(outs))],
        scratch_shapes=scratch,
        input_output_aliases=alias,
        cost_estimate=pl.CostEstimate(flops=flops, bytes_accessed=moved, transcendentals=0),
        compiler_params=pltpu.CompilerParams(vmem_limit_bytes=limit),
    )(*args)


def swap(value, axis, mask):
    count = lax.axis_size(axis)
    return lax.ppermute(value, axis, [(i, i ^ mask) for i in range(count)])


def pack_pair(value):
    high = value.astype(BF16).astype(F32)
    return high + pltpu.roll(value - high, HALF, 1)


def lane_of(shape):
    return lax.broadcasted_iota(jnp.int32, shape, 1)


def add_terms(terms):
    terms = [term.astype(F32) for term in terms]
    while len(terms) > 1:
        pairs = [a + b for a, b in zip(terms[::2], terms[1::2])]
        terms = pairs + terms[2 * len(pairs) :]
    return terms[0]


def residual(x_ref, terms, inner, group):
    total = add_terms([term[...] for term in terms])
    rows, cols = x_ref.shape
    own = rows // group
    span = cols // group
    blocks = []
    for block in range(group):
        tail = total[rows:, block * span : (block + 1) * span]
        square = tail[:, :1] + tail[:, span // 2 : span // 2 + 1]
        scale = lax.rsqrt(square / inner + EPS)
        part = slice(block * own, (block + 1) * own)
        blocks.append((x_ref[part, :].astype(F32) + scale * total[part, :]).astype(BF16))
    return blocks


def project(level, group, heads, source, gain, weights, step, keep_ref, send_ref, rows_ref, aux_ref):
    me = lax.axis_index("dp")
    first = lax.axis_index("tp") * heads
    rows, _ = source.shape
    own = rows // group
    half = group // 2
    order = [2 * k + 1 for k in range(half)] + [2 * k for k in range(half)]
    for slot, mask in enumerate(order):
        start = pl.multiple_of((me ^ mask) * own, own)
        rows_ref[slot * own : (slot + 1) * own, :] = source[pl.ds(start, own), :].astype(F32)
    values = rows_ref[...]
    gained = (values * gain[level : level + 1, :]).astype(BF16)
    square = jnp.sum(values * values, axis=1, keepdims=True)
    steps = lax.dot_general(gained, step(), (((1,), (1,)), ((), ())), preferred_element_type=F32)
    aux_ref[...] = jnp.zeros_like(aux_ref)
    aux_ref[:, : steps.shape[1]] = steps
    lane = lane_of((rows, LANES))
    steps = pltpu.roll(aux_ref[...], lax.rem(LANES - first, LANES), 1)
    packed = pack_pair(jnp.where(lane < heads, steps, jnp.where(lane == heads, square, 0.0)))
    middle = half * own
    at = 0
    for weight in weights:
        product = jnp.dot(gained, weight(), preferred_element_type=F32)
        width = product.shape[1]
        keep_ref[:, at : at + width] = product[:middle].astype(keep_ref.dtype)
        send_ref[:, at : at + width] = product[middle:].astype(BF16)
        at += width
    keep_ref[:, at:] = packed[:middle].astype(keep_ref.dtype)
    send_ref[:, at:] = packed[middle:].astype(BF16)


def first_kernel(level, group, heads, *refs):
    sources, (keep_ref, send_ref, x_out), rest = refs[:7], refs[7:10], refs[10:]
    rows_ref, aux_ref, sems, *buffers = rest
    buffers = [x_out, *buffers]
    copies = []
    for k, (source, buffer) in enumerate(zip(sources, buffers)):
        start = source if source.shape == buffer.shape else source.at[level]
        copies.append(pltpu.make_async_copy(start, buffer, sems.at[k]))
    for copy in copies:
        copy.start()

    def taker(k):
        def take():
            copies[k].wait()
            return buffers[k][...]

        return take

    copies[0].wait()
    copies[1].wait()
    weights = [taker(k) for k in range(3, 7)]
    project(
        level, group, heads, buffers[0], buffers[1], weights, taker(2), keep_ref, send_ref,
        rows_ref, aux_ref,
    )


def fetch_kernel(levels, count, *refs):
    sources, (recent_ref, taps_ref) = refs[1 : 1 + count], refs[1 + count : 3 + count]
    targets = refs[3 + count : 3 + 2 * count]
    recent_out, past_ref, last_ref, fold_ref, taps_scr, sems = refs[3 + 2 * count :]
    pairs = [(recent_ref, recent_out), (taps_ref, taps_scr)]
    for level, source, target in zip(levels, sources, targets):
        pairs.append((source if level is None else source.at[level], target))
    copies = [pltpu.make_async_copy(a, b, sems.at[k]) for k, (a, b) in enumerate(pairs)]
    for copy in copies:
        copy.start()
    cells, lanes = fold_ref.shape
    head_dim = lanes // 2
    step = 2 * lanes
    rows = lax.broadcasted_iota(jnp.int32, (step, lanes), 0) // (cells // head_dim)
    for block in range(cells // step):
        spot = lane_of((step, lanes)) % head_dim - block * (step * head_dim // cells)
        value = jnp.where(rows == spot, 1.0, 0.0).astype(BF16)
        fold_ref[block * step : (block + 1) * step, :] = value
    layers, own, kinds, old, channels = recent_ref.shape
    copies[0].wait()
    copies[1].wait()
    for level in range(layers):
        for kind in range(kinds):
            at = slice(kind * channels, (kind + 1) * channels)
            taps = [
                taps_scr[tap, kind].astype(F32)[level : level + 1] for tap in range(old + 1)
            ]
            last_ref[level : level + 1, at] = taps[old]
            taps = jnp.concatenate(taps[:old])
            for row in range(own):
                product = recent_out[level, row, kind].astype(F32) * taps
                past_ref[level, row : row + 1, at] = jnp.sum(product, axis=0, keepdims=True)
    for copy in copies[2:]:
        copy.wait()


def next_kernel(level, group, heads, inner, count, *refs):
    x_ref, terms = refs[0], refs[1 : 1 + count]
    step_ref, *weights, gain_ref = refs[1 + count : 7 + count]
    keep_ref, send_ref, x_out, rows_ref, aux_ref = refs[7 + count :]
    own = x_ref.shape[0] // group
    for block, value in enumerate(residual(x_ref, terms, inner, group)):
        x_out[block * own : (block + 1) * own, :] = value.astype(F32)
    project(
        level, group, heads, x_out, gain_ref, [lambda w=w: w[...] for w in weights],
        lambda: step_ref[...], keep_ref, send_ref, rows_ref, aux_ref,
    )


def chip_kernel(keep_ref, mate_ref, *outs):
    total = keep_ref[...].astype(F32) + mate_ref[...].astype(F32)
    own = outs[0].shape[0]
    body = total.shape[1] - LANES
    tail = total[:, body:]
    tail = tail + pltpu.roll(tail, HALF, 1)
    packed = pack_pair(jnp.where(lane_of(tail.shape) < HALF, tail, 0.0))
    for k, out in enumerate(outs):
        part = slice(k * own, (k + 1) * own)
        out[:, :body] = total[part, :body].astype(BF16)
        out[:, body:] = packed[part].astype(BF16)


def silu(value):
    return value / (1.0 + jnp.exp(-value))


def mixer_kernel(level, width, group, *refs):
    count = group // 2
    parts = refs[:count]
    (past_ref, last_ref, bias_ref, log_ref, skip_ref, gain_ref, fold_ref, state_ref) = refs[
        count : count + 8
    ]
    gated_ref, u_ref, x_out, b_out, d_out, prod_scr = refs[count + 8 :]
    _, heads, own, cells = state_ref.shape
    channels = gain_ref.shape[1]
    total = add_terms([part[...] for part in parts])
    aux = total[:, 4 * channels :]
    aux = aux + pltpu.roll(aux, HALF, 1)
    scale = lax.rsqrt(aux[:, heads : heads + 1] / width + EPS)
    gate = silu(scale * total[:, :channels])
    u = (scale * total[:, channels : 4 * channels]).astype(BF16)
    u_ref[...] = u
    act = silu(past_ref[level] + u.astype(F32) * last_ref[level : level + 1, :])
    raw = scale * aux[:, :heads] + bias_ref[level : level + 1, :]
    step = jnp.maximum(raw, 0.0) + jnp.log1p(jnp.exp(-jnp.abs(raw)))
    decay = jnp.exp(-step * jnp.exp(log_ref[level : level + 1, :]))
    low = lane_of((own, LANES)) < HALF
    mixed = []
    for head in range(heads):
        at = head // 2 * LANES
        odd = head % 2

        def doubled(offset):
            pair = act[:, offset + at : offset + at + LANES]
            turned = pltpu.roll(pair, HALF, 1)
            return jnp.where(low, turned, pair) if odd else jnp.where(low, pair, turned)

        xs, bs, cs = doubled(0), doubled(channels), doubled(2 * channels)
        ds = jnp.broadcast_to(decay[:, head : head + 1], (own, LANES))
        xd = xs * step[:, head : head + 1]
        x_out[head], b_out[head], d_out[head] = xd, bs, ds
        both = 0.5 * jnp.sum(bs * cs, axis=1, keepdims=True)
        mixed.append((ds, xd * both + xs * skip_ref[level : level + 1, head : head + 1]))
        for chunk in range(cells // LANES):
            span = slice(chunk * LANES, (chunk + 1) * LANES)
            prod_scr[head * own : (head + 1) * own, span] = state_ref[level, head, :, span] * cs
    y = jnp.dot(prod_scr[...].astype(BF16), fold_ref[...], preferred_element_type=F32)
    outs = [
        ds * y[head * own : (head + 1) * own] + add for head, (ds, add) in enumerate(mixed)
    ]
    for pair in range(channels // LANES):
        at = slice(pair * LANES, (pair + 1) * LANES)
        value = jnp.where(low, outs[2 * pair], outs[2 * pair + 1])
        out = (value * gate[:, at] * gain_ref[level : level + 1, at]).astype(BF16)
        for member in range(group):
            gated_ref[member, :, at] = out


def state_kernel(level, x_ref, b_ref, d_ref, state_ref, *refs):
    out_ref, fresh_scr, sems = refs[-3:]
    _, heads, own, cells = state_ref.shape
    pick = lane_of((own, LANES)) // HALF
    copies = []
    for head in range(heads):
        xs, bs, ds = x_ref[head], b_ref[head], d_ref[head]
        for chunk in range(cells // LANES):
            at = slice(chunk * LANES, (chunk + 1) * LANES)
            spread = jnp.take_along_axis(xs, pick + 2 * chunk, axis=1)
            fresh_scr[head, :, at] = ds * state_ref[level, head, :, at] + spread * bs
        copies.append(
            pltpu.make_async_copy(fresh_scr.at[head], out_ref.at[level, head], sems.at[head])
        )
        copies[-1].start()
    for copy in copies:
        copy.wait()


def recent_kernel(recent_ref, *refs):
    out_ref = refs[-1]
    layers, own, kinds, old, channels = recent_ref.shape
    for level in range(layers):
        u = refs[level][...].astype(F32)
        for row in range(own):
            for kind in range(kinds):
                rows = recent_ref[level, row, kind].astype(F32)
                fresh = u[row : row + 1, kind * channels : (kind + 1) * channels]
                out_ref[level, row, kind] = jnp.concatenate([rows[1:], fresh]).astype(BF16)


def out_kernel(level, group, gated_ref, weight_ref, out_ref):
    gated = gated_ref[...]
    rows = gated.shape[0]
    own = rows // group
    wide = gated.astype(F32)
    square = jnp.sum(wide * wide, axis=1, keepdims=True)
    product = jnp.dot(gated, weight_ref[level], preferred_element_type=F32)
    cols = product.shape[1]
    span = cols // group
    out_ref[:rows, :] = product.astype(BF16)
    lane = lane_of((own, cols))
    high = square.astype(BF16).astype(F32)
    low = square - high
    tail = jnp.zeros((own, cols), F32)
    for block in range(group):
        part = slice(block * own, (block + 1) * own)
        both = jnp.where(lane % span < span // 2, high[part], low[part])
        tail = jnp.where(lane // span == block, both, tail)
    out_ref[rows:, :] = tail.astype(BF16)


def last_kernel(inner, group, x_ref, *refs):
    own = x_ref.shape[0] // group
    for block, value in enumerate(residual(x_ref, refs[:-1], inner, group)):
        refs[-1][block * own : (block + 1) * own, :] = value


def shape(dims, dtype):
    return jax.ShapeDtypeStruct(dims, dtype)


def tp_terms(value):
    count = lax.axis_size("tp")
    if count & (count - 1) or count > 8:
        return [lax.psum(value.astype(F32), "tp")]
    terms = {0: value}
    for mask in sorted(range(1, count), reverse=True):
        terms[mask] = swap(value, "tp", mask)
    return [terms[mask] for mask in range(count)]


def per_device(
    tokens,
    norm_gain,
    w_gate,
    w_value,
    w_inmap,
    w_readout,
    w_step,
    step_bias,
    decay_log,
    skip_gain,
    conv_taps,
    gate_gain,
    w_project,
    states,
    recent,
):
    group = lax.axis_size("dp")
    rows, cols = tokens.shape
    width = cols * group
    layers, own, heads, cells = states.shape
    channels = w_gate.shape[2]
    inner = channels * lax.axis_size("tp")
    half = group // 2
    total = 4 * channels + LANES

    kinds = conv_taps.shape[2]
    states = states.transpose(0, 2, 1, 3)
    recent = recent.transpose(0, 1, 3, 2, 4)
    w_step = w_step.transpose(0, 2, 1)
    inputs = (w_gate, w_value, w_inmap, w_readout)
    later = [(w_step, 1), *((w, 1) for w in inputs), (norm_gain, None), (states, None)]
    later += [(w_project, None), (step_bias, None), (decay_log, None), (skip_gain, None)]
    later.append((gate_gain, None))
    flat = conv_taps.transpose(1, 2, 0, 3)

    def fetch(after):
        levels = [level for _, level in later]
        outs = [shape(a.shape if level is None else a.shape[1:], a.dtype) for a, level in later]
        outs += [
            shape(recent.shape, BF16),
            shape((layers, own, kinds * channels), F32),
            shape((layers, kinds * channels), F32),
            shape((cells, LANES), BF16),
        ]
        args = [after, *(a for a, _ in later), recent, flat]
        return call(
            functools.partial(fetch_kernel, levels, len(later)),
            outs,
            args,
            states.size * 8,
            [pltpu.VMEM(flat.shape, BF16), pltpu.SemaphoreType.DMA((len(args) - 1,))],
            far=range(1, len(args)),
        )

    terms = []
    fresh = []
    kept = []
    for level in range(layers):
        outs = [shape((half * own, total), F32), shape((half * own, total), BF16)]
        scratch = [pltpu.VMEM((rows, cols), F32), pltpu.VMEM((rows, LANES), F32)]
        if level:
            args = [current, *terms, *later_in]
            kernel = functools.partial(next_kernel, level, group, heads, inner, len(terms))
            outs.append(shape((rows, cols), F32))
            keep, send, current = call(kernel, outs, args, 2 * rows * cols * total, scratch)
        else:
            args = [tokens, norm_gain, w_step, *inputs]
            scratch.append(pltpu.SemaphoreType.DMA((len(args),)))
            dims = [a.shape if a.ndim == 2 else a.shape[1:] for a in args]
            scratch += [pltpu.VMEM(d, a.dtype) for d, a in zip(dims[1:], args[1:])]
            outs.append(shape((rows, cols), BF16))
            kernel = functools.partial(first_kernel, level, group, heads)
            keep, send, current = call(
                kernel, outs, args, 2 * rows * cols * total, scratch, far=range(len(args))
            )
        parts = call(
            chip_kernel,
            [shape((own, total), BF16)] * half,
            [keep, swap(send, "dp", 1)],
            half * own * total,
        )
        if not level:
            near = fetch(parts[0])
            later_in, (state_in, project_in, *small) = near[:6], near[6:12]
            recent_in, past, last, fold = near[12:]
        parts = [swap(parts[k], "dp", 2 * k + 1) for k in reversed(range(half))]
        gated, u, xd, bs, ds = call(
            functools.partial(mixer_kernel, level, width, group),
            [shape((group, own, channels), BF16), shape((own, kinds * channels), BF16)]
            + [shape((heads, own, LANES), F32)] * 3,
            [*parts, past, last, *small, fold, state_in],
            8 * own * heads * cells,
            [pltpu.VMEM((heads * own, cells), F32)],
        )
        every = lax.all_to_all(gated, "dp", 0, 0, tiled=True).reshape(rows, channels)
        fresh = call(
            functools.partial(state_kernel, level),
            [shape(states.shape, F32)],
            [xd, bs, ds, state_in, *fresh],
            8 * own * heads * cells,
            [pltpu.VMEM((heads, own, cells), F32), pltpu.SemaphoreType.DMA((heads,))],
            far=(4,),
            far_out=(0,),
            alias={4: 0} if fresh else {},
        )
        (product,) = call(
            functools.partial(out_kernel, level, group),
            [shape((rows + own, cols), BF16)],
            [every, project_in],
            2 * rows * channels * cols,
        )
        terms = tp_terms(product)
        kept.append(u)
    (current,) = call(
        functools.partial(last_kernel, inner, group),
        [shape((rows, cols), BF16)],
        [current, *terms],
        4 * rows * cols,
    )
    (kept,) = call(recent_kernel, [shape(recent.shape, BF16)], [recent_in, *kept], recent.size)
    return (current, fresh[0].transpose(0, 2, 1, 3), kept.transpose(0, 1, 3, 2, 4))


def solution(mesh):
    in_specs = (
        P(None, "dp"),
        P(None, "dp"),
        P(None, "dp", "tp"),
        P(None, "dp", "tp"),
        P(None, "dp", "tp"),
        P(None, "dp", "tp"),
        P(None, "dp", None),
        P(None, "tp"),
        P(None, "tp"),
        P(None, "tp"),
        P(None, None, None, "tp"),
        P(None, "tp"),
        P(None, "tp", "dp"),
        P(None, "dp", "tp", None),
        P(None, "dp", None, None, "tp"),
    )
    out_specs = (P(None, "dp"), P(None, "dp", "tp", None), P(None, "dp", None, None, "tp"))
    return jax.shard_map(
        per_device, mesh=mesh, in_specs=in_specs, out_specs=out_specs, check_vma=False
    )
```
